256 devices in a mesh: kv: 64 (over z, y, core), tp: 4 (over x).
Axes of the slice: x: 4, y: 4, z: 8, core: 2. Of those that a mesh axis runs over, the one named last changes fastest.
Arguments:
- tokens: bfloat16 [24576, 1024], P('kv', 'tp'), may hold values from -6 to 6
- query_weight: bfloat16 [1024, 512], P(None, 'tp'), may hold values from -0.1875 to 0.1875
- key_weight: bfloat16 [1024, 512], P(None, 'tp'), may hold values from -0.1875 to 0.1875
- value_weight: bfloat16 [1024, 512], P(None, 'tp'), may hold values from -0.1875 to 0.1875
- out_weight: bfloat16 [512, 1024], P('tp'), may hold values from -0.25 to 0.25
- norm_gain: float32 [512], P('tp'), may hold values from 0.1 to 1.9
- chosen_owner: int32 [384, 8], P('kv'), may hold values from 0 to 63, all different within a row; in each aligned block of 6 rows (0 to 5, 6 to 11, ...) at most 1 rows name the same one
- chosen_local: int32 [384, 8], P('kv'), may hold values from 0 to 5
Outputs:
- attended_out: bfloat16 [24576, 1024], P('kv', 'tp')
The draws below stay inside these ranges and needn't reach their ends.
Inputs may be any that keep to these rules, and one draw needn't show every extreme that they name: `chosen_owner`: each row names 8 different owners; among the 6 rows of one device no owner is named by more than 1 rows, and in some device's rows one owner is named by exactly 1. `chosen_local`: any index of a key block within its owner.
All inputs are finite; a program needn't handle non-finite values.
Results may differ from the reference program's by a relative error of at most 0.015.
Values may be sent and summed in bfloat16 or wider, within the bound.
No kernel may reach another device: no remote copies, remote signals or barrier semaphores. Data moves between devices by JAX's collectives and lax.ppermute only.
A program may use at most 64 MiB of HBM per device.

```python
import math
import jax
import jax.numpy as jnp
import numpy as np
from jax import lax

WIDTH = 1024
HEADS = 8
HEAD_SIZE = 64
BLOCK = 64
CHOSEN = 8
QB_DEV = 6
TOKENS = 24576
BLOCKS_ALL = 384
CAP = 1
N_KV = 64


def with_ends(drawn, key, least, high):
    shape = drawn.shape
    spot = [jax.random.randint(jax.random.fold_in(key, axis), (), 0, shape[axis]) for axis in range(len(shape))]
    drawn = drawn.at[tuple(spot)].set(least)
    longest = shape.index(max(shape))
    spot[longest] = (spot[longest] + 1) % shape[longest]
    return drawn.at[tuple(spot)].set(high)


def level_of(own_key, dims, split, least, largest):
    loudness = 1.0
    for axis_at, shards_of in split:
        draws = jax.random.uniform(jax.random.fold_in(jax.random.fold_in(own_key, 6), axis_at), (shards_of,), jnp.float32, least / len(split), largest / len(split))
        loudness = loudness * jnp.repeat(jnp.exp(draws), dims[axis_at] // shards_of).reshape((-1,) + (1,) * (len(dims) - 1 - axis_at))
    return loudness


def deal_out(key, own, number, rows, amount, top, most, lean):
    sequence = jax.random.permutation(key, amount)
    heavy_load, usual = shares(amount, rows * top, most, lean, True), shares(amount, rows * top, most, lean, False)
    places = jnp.arange(amount)

    def named(sizes, turn):
        used = int((sizes > 0).sum())
        fixed = max(1, used // 4)
        shifted = fixed + (places - fixed + turn * (used - fixed)) % max(1, amount - fixed)
        return jnp.zeros((amount,), jnp.int32).at[sequence[jnp.where(places < fixed, places, shifted)]].set(jnp.asarray(sizes, jnp.int32))

    sizes = jnp.where(number % 4 == 0, named(heavy_load, number // 4), named(usual, number - number // 4 - 1))
    mixed = jax.random.permutation(jax.random.fold_in(own, 3), amount)
    giver, receiver = mixed[0:amount // 2 * 2:2], mixed[1:amount // 2 * 2:2]
    margin = jnp.minimum(sizes[giver] - 1, most - sizes[receiver]) // 2
    margin = jnp.where((giver == sequence[0]) | (receiver == sequence[0]) | (sizes[receiver] == 0), 0, jnp.maximum(margin, 0))
    shifted = jax.random.randint(jax.random.fold_in(own, 4), (amount // 2,), 0, 1 << 20) % (margin + 1)
    sizes = sizes.at[giver].add(-shifted).at[receiver].add(shifted)
    items = jnp.searchsorted(jnp.cumsum(sizes), jnp.arange(rows * top), side="right").astype(jnp.int32)
    listing = items.reshape(top, rows).T
    listing = listing[jax.random.permutation(jax.random.fold_in(own, 1), rows)]
    turn = jax.random.randint(jax.random.fold_in(own, 2), (rows, 1), 0, top)
    return jnp.take_along_axis(listing, (jnp.arange(top)[None, :] + turn) % top, axis=1)


def shares(amount, total, reach, lean, full):
    weights = [(1 << 20) // math.isqrt(grade ** lean) + 1 for grade in range(1, amount + 1)]
    largest = reach if full else min(reach, max(-(-total // amount), total * weights[0] // sum(weights)))
    least = 1 if total - largest >= amount - 1 else 0
    counts, rest = [largest] + [least] * (amount - 1), total - largest - least * (amount - 1)
    while rest > 0:
        candidates = [i for i in range(1, amount) if counts[i] < largest] or [i for i in range(1, amount) if counts[i] < reach]
        mass, left = sum([weights[i] for i in candidates]), rest
        for i in candidates:
            more = min(reach - counts[i], max(1, left * weights[i] // mass), rest)
            counts[i] = counts[i] + more
            rest = rest - more
    return np.array(counts)


def noise(key, shape, scale, limit, shards=(), kind=jnp.bfloat16):
    array = scale * jax.random.normal(key, shape, jnp.float32)
    if shards:
        array = array * level_of(key, shape, shards, -0.22, 0.18)
    return jnp.clip(array, -limit, limit).astype(kind)


def setup_inputs(seed: int = 0) -> dict:
    keys = jax.random.split(jax.random.key(seed), 9)
    tokens = noise(keys[0], (TOKENS, WIDTH), 1.0, 6.0, ((0, 64), (1, 4)))
    query_weight = noise(keys[1], (WIDTH, HEADS * HEAD_SIZE), WIDTH ** -0.5, 0.1875, ((1, 4),))
    key_weight = noise(keys[2], (WIDTH, HEADS * HEAD_SIZE), WIDTH ** -0.5, 0.1875, ((1, 4),))
    value_weight = noise(keys[3], (WIDTH, HEADS * HEAD_SIZE), WIDTH ** -0.5, 0.1875, ((1, 4),))
    out_weight = noise(keys[4], (HEADS * HEAD_SIZE, WIDTH), (HEADS * HEAD_SIZE) ** -0.5, 0.25, ((0, 4),))
    norm_gain = jnp.clip(1.0 + 0.18 * jax.random.normal(keys[5], (HEADS * HEAD_SIZE,), jnp.float32), 0.1, 1.9)
    chosen_owner_keys = jax.random.split(jax.random.fold_in(keys[6], 1), BLOCKS_ALL // QB_DEV)
    chosen_owner_turns = jax.random.permutation(jax.random.fold_in(keys[6], 3), BLOCKS_ALL // QB_DEV)
    chosen_owner = jax.vmap(lambda own, number: deal_out(jax.random.fold_in(keys[6], 2), own, number, QB_DEV, N_KV, CHOSEN, CAP, 2))(chosen_owner_keys, chosen_owner_turns).reshape((BLOCKS_ALL, CHOSEN))
    chosen_local = with_ends(jax.random.randint(keys[7], (BLOCKS_ALL, CHOSEN), 0, QB_DEV), jax.random.fold_in(keys[7], 1), 0, QB_DEV - 1).astype(jnp.int32)
    return dict(tokens=tokens, query_weight=query_weight, key_weight=key_weight, value_weight=value_weight, out_weight=out_weight, norm_gain=norm_gain, chosen_owner=chosen_owner, chosen_local=chosen_local)


neg_fill = -1e+30
eps_norm = 1e-06

def project(tokens, weight):
    return jnp.dot(tokens, weight, preferred_element_type=jnp.float32).astype(jnp.bfloat16)

def reference(tokens, query_weight, key_weight, value_weight, out_weight, norm_gain, chosen_owner, chosen_local):
    block_count = QB_DEV * N_KV
    queries = project(tokens, query_weight).reshape(block_count, BLOCK, HEADS, HEAD_SIZE)
    keys_all = project(tokens, key_weight).reshape(block_count, BLOCK, HEADS, HEAD_SIZE)
    values_all = project(tokens, value_weight).reshape(block_count, BLOCK, HEADS, HEAD_SIZE)
    picked = (chosen_owner * QB_DEV + chosen_local).astype(jnp.int32)
    listed_all = jnp.concatenate([jnp.arange(block_count, dtype=jnp.int32)[:, None], picked], axis=1)
    offsets = jnp.arange(BLOCK, dtype=jnp.int32)
    score_scale = HEAD_SIZE ** (-0.5)
    entry_first = (jnp.arange(CHOSEN + 1, dtype=jnp.int32) == 0)[:, None]

    def attend(packed):
        block_index, listed = packed
        query_rows = queries[block_index].astype(jnp.float32)
        key_rows = keys_all[listed].astype(jnp.float32)
        value_rows = values_all[listed].astype(jnp.float32)
        scores = jnp.einsum('qhd,cthd->hqct', query_rows, key_rows, precision=lax.Precision.HIGHEST) * score_scale
        query_pos = block_index * BLOCK + offsets
        key_pos = jnp.where(entry_first, listed[:, None] * BLOCK + offsets[None, :], jnp.int32(-1))
        visible = key_pos[None, :, :] <= query_pos[:, None, None]
        scores = jnp.where(visible[None], scores, neg_fill)
        highest = lax.optimization_barrier(jnp.max(scores, axis=(2, 3), keepdims=True))
        weights = jnp.where(visible[None], jnp.exp(scores - highest), jnp.float32(0.0))
        mass_sum = lax.optimization_barrier(jnp.sum(weights, axis=(2, 3)))
        blended = jnp.einsum('hqct,cthd->qhd', weights, value_rows, precision=lax.Precision.HIGHEST)
        return (blended / mass_sum.T[:, :, None]).astype(jnp.bfloat16)
    attended = lax.map(attend, (jnp.arange(block_count, dtype=jnp.int32), listed_all))
    attended = attended.reshape(block_count * BLOCK, HEADS * HEAD_SIZE)
    wide_rows = attended.astype(jnp.float32)
    mean_sq = lax.optimization_barrier(jnp.mean(wide_rows * wide_rows, axis=1, keepdims=True))
    normed = (wide_rows * lax.rsqrt(mean_sq + eps_norm) * norm_gain.astype(jnp.float32)).astype(jnp.bfloat16)
    return jnp.dot(normed, out_weight, preferred_element_type=jnp.float32).astype(jnp.bfloat16)
```

```python
import functools

import jax
import jax.numpy as jnp
from jax import lax
from jax.experimental import pallas as pl
from jax.experimental.pallas import tpu as pltpu
from jax.sharding import Mesh
from jax.sharding import PartitionSpec as P

HEADS = 8
HEAD_SIZE = 64
BLOCK = 64
Z, Y, C, X = 8, 4, 2, 4

lowest = -1e30
eps_norm = 1e-06
VMEM = pltpu.VMEM
SMEM = pltpu.SMEM


def shift(n, s):
    return [(i, (i + s) % n) for i in range(n)]


def full(space=VMEM):
    return pl.BlockSpec(memory_space=space)


def head_turn(rows):
    turned = rows.T
    return jnp.concatenate([turned[:HEAD_SIZE], turned[HEAD_SIZE:]], axis=1)


def head_unturn(rows):
    return jnp.concatenate([rows[:, :HEAD_SIZE], rows[:, HEAD_SIZE:]], axis=0).T


def project_kernel(blocks, at, t0, t1, t2, t3, wq, wk, wv, q_out, k_out, v_out):
    pieces = [ref[...] for ref in (t0, t1, t2, t3)]
    starts = [pl.multiple_of(at[s] * 256, 256) for s in range(4)]

    def summed(weight):
        total = None
        for piece, start in zip(pieces, starts):
            term = jnp.dot(piece, weight[pl.ds(start, 256), :], preferred_element_type=jnp.float32)
            total = term if total is None else total + term
        return total

    k_out[...] = summed(wk).astype(jnp.bfloat16)
    values = summed(wv)
    for b in range(blocks):
        v_out[b * 64 : b * 64 + 64, :] = head_turn(values[b * 64 : b * 64 + 64]).astype(jnp.bfloat16)
    queries = summed(wq).astype(jnp.bfloat16).astype(jnp.float32) * (HEAD_SIZE ** (-0.5))
    for b in range(blocks):
        q_out[b * 64 : b * 64 + 64, :] = head_turn(queries[b * 64 : b * 64 + 64]).astype(
            jnp.bfloat16
        )


def project(at, pieces, weights):
    rows = pieces[0].shape[0]
    out = jax.ShapeDtypeStruct((rows, 128), jnp.bfloat16)
    return pl.pallas_call(
        functools.partial(project_kernel, rows // BLOCK),
        out_shape=(out, out, out),
        in_specs=[full(SMEM)] + [full()] * 7,
        out_specs=(full(),) * 3,
        name="project",
    )(at, *pieces, *weights)


def spread_heads(rows, lane):
    none = jnp.zeros_like(rows)
    return jnp.concatenate(
        [jnp.where(lane < HEAD_SIZE, rows, none), jnp.where(lane < HEAD_SIZE, none, rows)], axis=0
    )


def one_pair(q, k, v, lane, mask=None):
    scores = jnp.dot(k, spread_heads(q, lane), preferred_element_type=jnp.float32)
    if mask is not None:
        scores = jnp.where(mask, scores, lowest)
    highest = jnp.max(scores, axis=0, keepdims=True)
    weights = jnp.exp(scores - highest)
    mass = jnp.sum(weights, axis=0, keepdims=True)
    blended = jnp.dot(
        v, spread_heads(weights.astype(jnp.bfloat16), lane), preferred_element_type=jnp.float32
    )
    return highest, mass, blended


def attend_kernel(blocks, owners, first, last, *refs):
    refs = list(refs)
    table = refs.pop(0)
    q = [refs.pop(0) for _ in range(Y)]
    kv = [(refs.pop(0), refs.pop(0)) for _ in range(owners)]
    carry = None if first else [refs.pop(0) for _ in range(3)]
    if last:
        out = [refs.pop(0) for _ in range(Y)]
    top, mass, total = refs
    lane = lax.broadcasted_iota(jnp.int32, (BLOCK, 128), 1)

    if first:
        for g in range(blocks, Y * blocks):
            top[g] = jnp.full((8, 128), lowest, jnp.float32)
            mass[g] = jnp.zeros((8, 128), jnp.float32)
            total[g] = jnp.zeros((BLOCK, 128), jnp.float32)
        spot = lax.broadcasted_iota(jnp.int32, (BLOCK, 128), 0)
        seen = spot <= (lane & (HEAD_SIZE - 1))
        for b in range(blocks):
            here = slice(b * 64, b * 64 + 64)
            m, l, o = one_pair(q[0][here, :], kv[0][0][here, :], kv[0][1][here, :], lane, seen)
            top[b] = jnp.broadcast_to(m, (8, 128))
            mass[b] = jnp.broadcast_to(l, (8, 128))
            total[b] = o
    else:
        for src, dst in zip(carry, (top, mass, total)):
            dst[...] = src[...]

    for owner in range(owners):
        found = []
        for p in range(Y):
            code = table[owner * Y + p]
            row = jnp.maximum(code - 1, 0)
            local = pl.multiple_of((row & 7) * BLOCK, BLOCK)
            row = row >> 3
            m, l, o = one_pair(
                q[p][pl.ds(pl.multiple_of(row * BLOCK, BLOCK), BLOCK), :],
                kv[owner][0][pl.ds(local, BLOCK), :],
                kv[owner][1][pl.ds(local, BLOCK), :],
                lane,
            )
            found.append((code > 0, p * blocks + row, m, l, o))
        for real, g, m, l, o in found:
            m = jnp.where(real, m, lowest)
            before = top[g]
            now = jnp.maximum(before, m)
            keep = jnp.exp(before - now)
            add = jnp.where(real, jnp.exp(m - now), 0.0)
            top[g] = now
            mass[g] = mass[g] * keep + l * add
            total[g] = total[g] * keep[:1] + o * add[:1]

    if last:
        line = lax.broadcasted_iota(jnp.int32, (8, 128), 0)
        for p in range(Y):
            stats = []
            for b in range(blocks):
                g = p * blocks + b
                out[p][b * 64 : b * 64 + 64, :] = total[g].astype(jnp.bfloat16)
                tile = jnp.zeros((8, 128), jnp.float32)
                for at, value in ((0, top[g]), (3, mass[g])):
                    for i in range(3):
                        part = value.astype(jnp.bfloat16).astype(jnp.float32)
                        tile = jnp.where(line == at + i, part, tile)
                        value = value - part
                stats.append(tile)
            out[p][blocks * 64 :, :] = jnp.concatenate(stats, axis=0).astype(jnp.bfloat16)


def attend(table, q, kv, carry, last):
    rows = q[0].shape[0]
    blocks = rows // BLOCK
    groups = Y * blocks
    state = [
        jax.ShapeDtypeStruct((groups, 8, 128), jnp.float32),
        jax.ShapeDtypeStruct((groups, 8, 128), jnp.float32),
        jax.ShapeDtypeStruct((groups, BLOCK, 128), jnp.float32),
    ]
    if last:
        outs = [jax.ShapeDtypeStruct((rows + 8 * blocks, 128), jnp.bfloat16)] * Y
        scratch = [VMEM(s.shape, s.dtype) for s in state]
    else:
        outs, scratch = state, []
    args = [table, *q]
    for pair in kv:
        args += list(pair)
    if carry is not None:
        args += list(carry)
    return pl.pallas_call(
        functools.partial(attend_kernel, blocks, len(kv), carry is None, last),
        out_shape=tuple(outs),
        in_specs=[full(SMEM)] + [full()] * (len(args) - 1),
        out_specs=(full(),) * len(outs),
        scratch_shapes=scratch,
        name="attend_late" if last else "attend_early",
    )(*args)


def merge_kernel(blocks, *refs):
    parts, out = refs[:-1], refs[-1]
    stats = [part[blocks * 64 :, :].astype(jnp.float32) for part in parts]
    for b in range(blocks):
        tops, masses = [], []
        for s in stats:
            t = s[b * 8 : b * 8 + 8]
            tops.append(t[0:1] + t[1:2] + t[2:3])
            masses.append(t[3:4] + t[4:5] + t[5:6])
        highest = functools.reduce(jnp.maximum, tops)
        mass, blended = 0.0, 0.0
        for part, m, l in zip(parts, tops, masses):
            scale = jnp.exp(m - highest)
            mass = mass + l * scale
            blended = blended + part[b * 64 : b * 64 + 64, :].astype(jnp.float32) * scale
        out[b * 64 : b * 64 + 64, :] = head_unturn(blended / mass).astype(jnp.bfloat16)


def merge(parts, blocks):
    return pl.pallas_call(
        functools.partial(merge_kernel, blocks),
        out_shape=jax.ShapeDtypeStruct((blocks * BLOCK, 128), jnp.bfloat16),
        in_specs=[full()] * len(parts),
        out_specs=full(),
        name="merge",
    )(*parts)


def finish_kernel(a0, a1, a2, a3, w0, w1, w2, w3, out):
    squares, summed = None, None
    for a, w in ((a0, w0), (a1, w1), (a2, w2), (a3, w3)):
        rows = a[...]
        wide = rows.astype(jnp.float32)
        term = jnp.dot(rows, w[...], preferred_element_type=jnp.float32)
        squares = wide * wide if squares is None else squares + wide * wide
        summed = term if summed is None else summed + term
    mean_sq = jnp.sum(squares, axis=1, keepdims=True) / (HEADS * HEAD_SIZE)
    out[...] = (summed * lax.rsqrt(mean_sq + eps_norm)).astype(jnp.bfloat16)


def finish(pieces, weights):
    rows, cols = pieces[0].shape[0], weights[0].shape[1]
    return pl.pallas_call(
        finish_kernel,
        out_shape=jax.ShapeDtypeStruct((rows, cols), jnp.bfloat16),
        in_specs=[full()] * 8,
        out_specs=full(),
        name="finish",
    )(*pieces, *weights)


def on_device(
    tokens,
    query_weight,
    key_weight,
    value_weight,
    out_weight,
    norm_gain,
    chosen_owner,
    chosen_local,
):
    rows = tokens.shape[0]
    blocks = rows // BLOCK
    x, z, y, c = (lax.axis_index(name) for name in ("x", "z", "y", "c"))

    pieces = [tokens] + [lax.ppermute(tokens, "x", shift(X, s)) for s in (1, 2, 3)]
    at = jnp.stack([(x - s) % X for s in range(X)]).astype(jnp.int32)

    picked = chosen_owner * 8 + chosen_local
    picks = [picked] + [lax.ppermute(picked, "y", shift(Y, s)) for s in (1, 2, 3)]

    q, k, v = project(at, pieces, (query_weight, key_weight, value_weight))

    swap = [(0, 1), (1, 0)]
    own = {0: (k, v)}
    up, down = (k, v), (k, v)
    for step in range(1, Z // 2):
        up = tuple(lax.ppermute(a, "z", shift(Z, 1)) for a in up)
        down = tuple(lax.ppermute(a, "z", shift(Z, -1)) for a in down)
        own[-step], own[step] = up, down
    own[Z // 2] = (lax.ppermute(up[0], "z", shift(Z, 1)), lax.ppermute(down[1], "z", shift(Z, -1)))
    other = {d: tuple(lax.ppermute(a, "c", swap) for a in pair) for d, pair in own.items()}

    queries = [q] + [lax.ppermute(q, "y", shift(Y, s)) for s in (1, 2, 3)]

    order = [0, -1, 1, -2, 2, -3, 3, Z // 2]
    column = jnp.stack(
        [((z + d) % Z) * (Y * C) + y * C + (c ^ cc) for d in order for cc in (0, 1)]
    ).astype(jnp.int32)
    picks = jnp.stack(picks)
    code = 1 + 8 * jnp.arange(blocks, dtype=jnp.int32)[None, :, None] + (picks & 7)
    hit = (picks >> 3)[None] == column[:, None, None, None]
    table = jnp.sum(jnp.where(hit, code[None], 0), axis=(2, 3)).reshape(-1)

    kv = []
    for d in order:
        kv += [own[d], other[d]]
    early = 10
    carry = attend(table[: early * Y], queries, kv[:early], None, False)
    parts = attend(table[early * Y :], queries, kv[early:], carry, True)

    back = [parts[0]] + [lax.ppermute(parts[s], "y", shift(Y, -s)) for s in (1, 2, 3)]
    attended = merge(back, blocks)

    width = out_weight.shape[1] // X
    gained = []
    for s in range(X):
        columns = lax.dynamic_slice_in_dim(out_weight, ((x + s) % X) * width, width, 1)
        gained.append((columns.astype(jnp.float32) * norm_gain[:, None]).astype(jnp.bfloat16))
    weights = [gained[0]] + [lax.ppermute(gained[s], "x", shift(X, s)) for s in (1, 2, 3)]
    spread = [attended] + [lax.ppermute(attended, "x", shift(X, s)) for s in (1, 2, 3)]
    return finish(spread, weights)


def solution(mesh):
    fine = Mesh(mesh.devices.reshape(Z, Y, C, X), ("z", "y", "c", "x"))
    kv = ("z", "y", "c")
    return jax.shard_map(
        on_device,
        mesh=fine,
        in_specs=(
            P(kv, "x"),
            P(None, "x"),
            P(None, "x"),
            P(None, "x"),
            P("x", None),
            P("x"),
            P(kv, None),
            P(kv, None),
        ),
        out_specs=P(kv, "x"),
        check_vma=False,
    )
```

```python
import functools

import jax
import jax.numpy as jnp
from jax import lax
from jax.experimental import pallas as pl
from jax.experimental.pallas import tpu as pltpu
from jax.sharding import Mesh
from jax.sharding import PartitionSpec as P

HEADS = 8
HEAD_SIZE = 64
BLOCK = 64
Z, Y, C, X = 8, 4, 2, 4

lowest = -1e30
eps_norm = 1e-06
VMEM = pltpu.VMEM
SMEM = pltpu.SMEM


def vmem(a):
    return pltpu.with_memory_space_constraint(a, VMEM)


def shift(n, s):
    return [(i, (i + s) % n) for i in range(n)]


def full(space=VMEM):
    return pl.BlockSpec(memory_space=space)


def head_turn(rows):
    turned = rows.T
    return jnp.concatenate([turned[:HEAD_SIZE], turned[HEAD_SIZE:]], axis=1)


def head_unturn(rows):
    return jnp.concatenate([rows[:, :HEAD_SIZE], rows[:, HEAD_SIZE:]], axis=0).T


def project_kernel(blocks, at, t0, t1, t2, t3, wq, wk, wv, q_out, kv_out):
    pieces = [ref[...] for ref in (t0, t1, t2, t3)]
    starts = [pl.multiple_of(at[s] * 256, 256) for s in range(4)]

    def summed(weight):
        total = None
        for piece, start in zip(pieces, starts):
            term = jnp.dot(piece, weight[pl.ds(start, 256), :], preferred_element_type=jnp.float32)
            total = term if total is None else total + term
        return total

    half = blocks * BLOCK
    kv_out[:half, :] = summed(wk).astype(jnp.bfloat16)
    values = summed(wv)
    for b in range(blocks):
        turned = head_turn(values[b * 64 : b * 64 + 64])
        kv_out[half + b * 64 : half + b * 64 + 64, :] = turned.astype(jnp.bfloat16)
    queries = summed(wq).astype(jnp.bfloat16).astype(jnp.float32) * (HEAD_SIZE ** (-0.5))
    for b in range(blocks):
        q_out[b * 64 : b * 64 + 64, :] = head_turn(queries[b * 64 : b * 64 + 64]).astype(
            jnp.bfloat16
        )


def project(at, pieces, weights):
    rows = pieces[0].shape[0]
    return pl.pallas_call(
        functools.partial(project_kernel, rows // BLOCK),
        out_shape=(VMEM((rows, 128), jnp.bfloat16), VMEM((2 * rows, 128), jnp.bfloat16)),
        in_specs=[full(SMEM)] + [full()] * 7,
        out_specs=(full(),) * 2,
        name="project",
    )(at, *[vmem(a) for a in (*pieces, *weights)])


def spread_heads(rows, lane):
    none = jnp.zeros_like(rows)
    return jnp.concatenate(
        [jnp.where(lane < HEAD_SIZE, rows, none), jnp.where(lane < HEAD_SIZE, none, rows)], axis=0
    )


def one_pair(q, k, v, lane, mask=None):
    scores = jnp.dot(k, spread_heads(q, lane), preferred_element_type=jnp.float32)
    if mask is not None:
        scores = jnp.where(mask, scores, lowest)
    highest = jnp.max(scores, axis=0, keepdims=True)
    weights = jnp.exp(scores - highest)
    mass = jnp.sum(weights, axis=0, keepdims=True)
    blended = jnp.dot(
        v, spread_heads(weights.astype(jnp.bfloat16), lane), preferred_element_type=jnp.float32
    )
    return highest, mass, blended


def attend_kernel(blocks, owners, first, last, *refs):
    refs = list(refs)
    table = refs.pop(0)
    q = [refs.pop(0) for _ in range(Y)]
    kv = [refs.pop(0) for _ in range(owners)]
    half = blocks * BLOCK
    carry = None if first else [refs.pop(0) for _ in range(3)]
    if last:
        out = [refs.pop(0) for _ in range(Y)]
    top, mass, total = refs
    lane = lax.broadcasted_iota(jnp.int32, (BLOCK, 128), 1)

    if first:
        for g in range(blocks, Y * blocks):
            top[g] = jnp.full((8, 128), lowest, jnp.float32)
            mass[g] = jnp.zeros((8, 128), jnp.float32)
            total[g] = jnp.zeros((BLOCK, 128), jnp.float32)
        spot = lax.broadcasted_iota(jnp.int32, (BLOCK, 128), 0)
        seen = spot <= (lane & (HEAD_SIZE - 1))
        for b in range(blocks):
            here = slice(b * 64, b * 64 + 64)
            after = slice(half + b * 64, half + b * 64 + 64)
            m, l, o = one_pair(q[0][here, :], kv[0][here, :], kv[0][after, :], lane, seen)
            top[b] = jnp.broadcast_to(m, (8, 128))
            mass[b] = jnp.broadcast_to(l, (8, 128))
            total[b] = o
    else:
        for src, dst in zip(carry, (top, mass, total)):
            dst[...] = src[...]

    for owner in range(owners):
        found = []
        for p in range(Y):
            code = table[owner * Y + p]
            row = jnp.maximum(code - 1, 0)
            local = pl.multiple_of((row & 7) * BLOCK, BLOCK)
            row = row >> 3
            m, l, o = one_pair(
                q[p][pl.ds(pl.multiple_of(row * BLOCK, BLOCK), BLOCK), :],
                kv[owner][pl.ds(local, BLOCK), :],
                kv[owner][pl.ds(half + local, BLOCK), :],
                lane,
            )
            found.append((code > 0, p * blocks + row, m, l, o))
        for real, g, m, l, o in found:
            m = jnp.where(real, m, lowest)
            before = top[g]
            now = jnp.maximum(before, m)
            keep = jnp.exp(before - now)
            add = jnp.where(real, jnp.exp(m - now), 0.0)
            top[g] = now
            mass[g] = mass[g] * keep + l * add
            total[g] = total[g] * keep[:1] + o * add[:1]

    if last:
        line = lax.broadcasted_iota(jnp.int32, (8, 128), 0)
        for p in range(Y):
            stats = []
            for b in range(blocks):
                g = p * blocks + b
                out[p][b * 64 : b * 64 + 64, :] = total[g].astype(jnp.bfloat16)
                tile = jnp.zeros((8, 128), jnp.float32)
                for at, value in ((0, top[g]), (3, mass[g])):
                    for i in range(3):
                        part = value.astype(jnp.bfloat16).astype(jnp.float32)
                        tile = jnp.where(line == at + i, part, tile)
                        value = value - part
                stats.append(tile)
            out[p][blocks * 64 :, :] = jnp.concatenate(stats, axis=0).astype(jnp.bfloat16)


def attend(table, q, kv, carry, last):
    rows = q[0].shape[0]
    blocks = rows // BLOCK
    groups = Y * blocks
    state = [
        jax.ShapeDtypeStruct((groups, 8, 128), jnp.float32),
        jax.ShapeDtypeStruct((groups, 8, 128), jnp.float32),
        jax.ShapeDtypeStruct((groups, BLOCK, 128), jnp.float32),
    ]
    if last:
        outs = [jax.ShapeDtypeStruct((rows + 8 * blocks, 128), jnp.bfloat16)] * Y
        scratch = [VMEM(s.shape, s.dtype) for s in state]
    else:
        outs, scratch = state, []
    outs = [VMEM(s.shape, s.dtype) for s in outs]
    args = [table] + [vmem(a) for a in (*q, *kv, *(carry or ()))]
    return pl.pallas_call(
        functools.partial(attend_kernel, blocks, len(kv), carry is None, last),
        out_shape=tuple(outs),
        in_specs=[full(SMEM)] + [full()] * (len(args) - 1),
        out_specs=(full(),) * len(outs),
        scratch_shapes=scratch,
        name="attend_late" if last else "attend_early",
    )(*args)


def merge_kernel(blocks, *refs):
    parts, out = refs[:-1], refs[-1]
    stats = [part[blocks * 64 :, :].astype(jnp.float32) for part in parts]
    for b in range(blocks):
        tops, masses = [], []
        for s in stats:
            t = s[b * 8 : b * 8 + 8]
            tops.append(t[0:1] + t[1:2] + t[2:3])
            masses.append(t[3:4] + t[4:5] + t[5:6])
        highest = functools.reduce(jnp.maximum, tops)
        mass, blended = 0.0, 0.0
        for part, m, l in zip(parts, tops, masses):
            scale = jnp.exp(m - highest)
            mass = mass + l * scale
            blended = blended + part[b * 64 : b * 64 + 64, :].astype(jnp.float32) * scale
        out[b * 64 : b * 64 + 64, :] = head_unturn(blended / mass).astype(jnp.bfloat16)


def merge(parts, blocks):
    return pl.pallas_call(
        functools.partial(merge_kernel, blocks),
        out_shape=VMEM((blocks * BLOCK, 128), jnp.bfloat16),
        in_specs=[full()] * len(parts),
        out_specs=full(),
        name="merge",
    )(*[vmem(a) for a in parts])


def finish_kernel(a0, a1, a2, a3, w0, w1, w2, w3, out):
    squares, summed = None, None
    for a, w in ((a0, w0), (a1, w1), (a2, w2), (a3, w3)):
        rows = a[...]
        wide = rows.astype(jnp.float32)
        term = jnp.dot(rows, w[...], preferred_element_type=jnp.float32)
        squares = wide * wide if squares is None else squares + wide * wide
        summed = term if summed is None else summed + term
    mean_sq = jnp.sum(squares, axis=1, keepdims=True) / (HEADS * HEAD_SIZE)
    out[...] = (summed * lax.rsqrt(mean_sq + eps_norm)).astype(jnp.bfloat16)


def finish(pieces, weights):
    rows, cols = pieces[0].shape[0], weights[0].shape[1]
    return pl.pallas_call(
        finish_kernel,
        out_shape=jax.ShapeDtypeStruct((rows, cols), jnp.bfloat16),
        in_specs=[full()] * 8,
        out_specs=full(),
        name="finish",
    )(*[vmem(a) for a in (*pieces, *weights)])


def on_device(
    tokens,
    query_weight,
    key_weight,
    value_weight,
    out_weight,
    norm_gain,
    chosen_owner,
    chosen_local,
):
    rows = tokens.shape[0]
    blocks = rows // BLOCK
    x, z, y, c = (lax.axis_index(name) for name in ("x", "z", "y", "c"))

    pieces = [tokens] + [lax.ppermute(tokens, "x", shift(X, s)) for s in (1, 2, 3)]
    at = jnp.stack([(x - s) % X for s in range(X)]).astype(jnp.int32)

    picked = chosen_owner * 8 + chosen_local
    picks = [picked] + [lax.ppermute(picked, "y", shift(Y, s)) for s in (1, 2, 3)]

    width = out_weight.shape[1] // X
    gained = []
    for s in range(X):
        columns = lax.dynamic_slice_in_dim(out_weight, ((x + s) % X) * width, width, 1)
        gained.append((columns.astype(jnp.float32) * norm_gain[:, None]).astype(jnp.bfloat16))
    weights = [gained[0]] + [lax.ppermute(gained[s], "x", shift(X, s)) for s in (1, 2, 3)]

    q, kv = project(at, pieces, (query_weight, key_weight, value_weight))

    places = [(i, j) for i in range(Z) for j in range(C)]

    def onward(k):
        return [(C * i + j, C * ((i + (k if j == 0 else -k)) % Z) + j) for i, j in places]

    def swap(a):
        return lax.ppermute(a, "c", [(0, 1), (1, 0)])

    same, cross = [kv], [swap(kv)]
    held = [(0, 0, kv), (0, 1, cross[0])]
    for step in (1, 2, 3):
        same.append(lax.ppermute(same[-1], ("z", "c"), onward(1)))
        cross.append(lax.ppermute(cross[-1], ("z", "c"), onward(1)))
        held += [(step, 0, same[-1]), (step, 1, cross[-1])]
        held += [(-step, 1, swap(same[-1])), (-step, 0, swap(cross[-1]))]
    far = lax.ppermute(same[2], ("z", "c"), onward(2))
    held += [(4, 0, far), (4, 1, swap(far))]

    queries = [q] + [lax.ppermute(q, "y", shift(Y, s)) for s in (1, 2, 3)]

    toward = 2 * c - 1
    column = jnp.stack(
        [((z + toward * d) % Z) * (Y * C) + y * C + (c ^ cc) for d, cc, _ in held]
    ).astype(jnp.int32)
    picks = jnp.stack(picks)
    code = 1 + 8 * jnp.arange(blocks, dtype=jnp.int32)[None, :, None] + (picks & 7)
    hit = (picks >> 3)[None] == column[:, None, None, None]
    table = jnp.sum(jnp.where(hit, code[None], 0), axis=(2, 3)).reshape(-1)

    early = 10
    arrays = [a for _, _, a in held]
    carry = attend(table[: early * Y], queries, arrays[:early], None, False)
    parts = attend(table[early * Y :], queries, arrays[early:], carry, True)

    back = [parts[0]] + [lax.ppermute(parts[s], "y", shift(Y, -s)) for s in (1, 2, 3)]
    attended = merge(back, blocks)
    spread = [attended] + [lax.ppermute(attended, "x", shift(X, s)) for s in (1, 2, 3)]
    return finish(spread, weights)


def solution(mesh):
    fine = Mesh(mesh.devices.reshape(Z, Y, C, X), ("z", "y", "c", "x"))
    kv = ("z", "y", "c")
    return jax.shard_map(
        on_device,
        mesh=fine,
        in_specs=(
            P(kv, "x"),
            P(None, "x"),
            P(None, "x"),
            P(None, "x"),
            P("x", None),
            P("x"),
            P(kv, None),
            P(kv, None),
        ),
        out_specs=P(kv, "x"),
        check_vma=False,
    )
```

```python
import functools

import jax
import jax.numpy as jnp
from jax import lax
from jax.experimental import pallas as pl
from jax.experimental.pallas import tpu as pltpu
from jax.sharding import Mesh
from jax.sharding import PartitionSpec as P

HEADS = 8
HEAD_SIZE = 64
BLOCK = 64
Z, Y, C, X = 8, 4, 2, 4

lowest = -1e30
eps_norm = 1e-06
VMEM = pltpu.VMEM
SMEM = pltpu.SMEM


PARAMS = pltpu.CompilerParams(vmem_limit_bytes=16 * 1024 * 1024)


def vmem(a):
    return pltpu.with_memory_space_constraint(a, VMEM)


def shift(n, s):
    return [(i, (i + s) % n) for i in range(n)]


def full(space=VMEM):
    return pl.BlockSpec(memory_space=space)


def head_turn(rows):
    turned = rows.T
    return jnp.concatenate([turned[:HEAD_SIZE], turned[HEAD_SIZE:]], axis=1)


def head_unturn(rows):
    return jnp.concatenate([rows[:, :HEAD_SIZE], rows[:, HEAD_SIZE:]], axis=0).T


def stage_kernel(tokens, wq, wk, wv, tokens_out, w_out):
    tokens_out[...] = tokens[...]
    for i, ref in enumerate((wq, wk, wv)):
        w_out[:, i * 128 : i * 128 + 128] = ref[...]


def stage(tokens, weights):
    depth, width = weights[0].shape
    return pl.pallas_call(
        stage_kernel,
        out_shape=(
            VMEM(tokens.shape, tokens.dtype),
            VMEM((depth, 3 * width), jnp.bfloat16),
        ),
        in_specs=[full()] * 4,
        out_specs=(full(),) * 2,
        name="stage",
        compiler_params=PARAMS,
    )(*[pltpu.with_memory_space_constraint(a, pltpu.HBM) for a in (tokens, *weights)])


def project_kernel(blocks, at, t0, t1, t2, t3, weight, q_out, kv_out):
    total = None
    for s, piece in enumerate((t0, t1, t2, t3)):
        start = pl.multiple_of(at[s] * 256, 256)
        term = jnp.dot(
            piece[...], weight[pl.ds(start, 256), :], preferred_element_type=jnp.float32
        )
        total = term if total is None else total + term
    half = blocks * BLOCK
    kv_out[:half, :] = total[:, 128:256].astype(jnp.bfloat16)
    queries = total[:, :128].astype(jnp.bfloat16).astype(jnp.float32) * (HEAD_SIZE ** (-0.5))
    values = total[:, 256:]
    for b in range(blocks):
        here = slice(b * 64, b * 64 + 64)
        kv_out[half + b * 64 : half + b * 64 + 64, :] = head_turn(values[here]).astype(jnp.bfloat16)
        q_out[here, :] = head_turn(queries[here]).astype(jnp.bfloat16)


def project(at, pieces, weight):
    rows = pieces[0].shape[0]
    return pl.pallas_call(
        functools.partial(project_kernel, rows // BLOCK),
        out_shape=(VMEM((rows, 128), jnp.bfloat16), VMEM((2 * rows, 128), jnp.bfloat16)),
        in_specs=[full(SMEM)] + [full()] * 5,
        out_specs=(full(),) * 2,
        name="project",
        compiler_params=PARAMS,
    )(at, *[vmem(a) for a in (*pieces, weight)])


def spread_heads(rows, lane):
    none = jnp.zeros_like(rows)
    return jnp.concatenate(
        [jnp.where(lane < HEAD_SIZE, rows, none), jnp.where(lane < HEAD_SIZE, none, rows)], axis=0
    )


def one_pair(q, k, v, lane, mask=None):
    scores = jnp.dot(k, spread_heads(q, lane), preferred_element_type=jnp.float32)
    if mask is not None:
        scores = jnp.where(mask, scores, lowest)
    highest = jnp.max(scores, axis=0, keepdims=True)
    weights = jnp.exp(scores - highest)
    mass = jnp.sum(weights, axis=0, keepdims=True)
    blended = jnp.dot(
        v, spread_heads(weights.astype(jnp.bfloat16), lane), preferred_element_type=jnp.float32
    )
    return highest, mass, blended


def attend_kernel(blocks, owners, begin, last, *refs):
    refs = list(refs)
    first = begin == 0
    table = refs.pop(0)
    q = [refs.pop(0) for _ in range(Y)]
    kv = [refs.pop(0) for _ in range(owners)]
    half = blocks * BLOCK
    carry = None if first else refs.pop(0)
    if last:
        out = [refs.pop(0) for _ in range(Y)]
    (state,) = refs
    total, top, mass = (state.at[:, a:b, :] for a, b in ((0, 64), (64, 72), (72, 80)))
    lane = lax.broadcasted_iota(jnp.int32, (BLOCK, 128), 1)

    if first:
        for g in range(blocks, Y * blocks):
            top[g] = jnp.full((8, 128), lowest, jnp.float32)
            mass[g] = jnp.zeros((8, 128), jnp.float32)
            total[g] = jnp.zeros((BLOCK, 128), jnp.float32)
        spot = lax.broadcasted_iota(jnp.int32, (BLOCK, 128), 0)
        seen = spot <= (lane & (HEAD_SIZE - 1))
        for b in range(blocks):
            here = slice(b * 64, b * 64 + 64)
            after = slice(half + b * 64, half + b * 64 + 64)
            m, l, o = one_pair(q[0][here, :], kv[0][here, :], kv[0][after, :], lane, seen)
            top[b] = jnp.broadcast_to(m, (8, 128))
            mass[b] = jnp.broadcast_to(l, (8, 128))
            total[b] = o
    else:
        state[...] = carry[...]

    for owner in range(owners):
        found = []
        for p in range(Y):
            code = table[p * (Z * C) + begin + owner]
            row = jnp.maximum(code - 1, 0)
            local = pl.multiple_of((row & 7) * BLOCK, BLOCK)
            row = row >> 3
            m, l, o = one_pair(
                q[p][pl.ds(pl.multiple_of(row * BLOCK, BLOCK), BLOCK), :],
                kv[owner][pl.ds(local, BLOCK), :],
                kv[owner][pl.ds(half + local, BLOCK), :],
                lane,
            )
            found.append((code > 0, p * blocks + row, m, l, o))
        for real, g, m, l, o in found:
            m = jnp.where(real, m, lowest)
            before = top[g]
            now = jnp.maximum(before, m)
            keep = jnp.exp(before - now)
            add = jnp.where(real, jnp.exp(m - now), 0.0)
            top[g] = now
            mass[g] = mass[g] * keep + l * add
            total[g] = total[g] * keep[:1] + o * add[:1]

    if last:
        line = lax.broadcasted_iota(jnp.int32, (8, 128), 0)
        for p in range(Y):
            stats = []
            for b in range(blocks):
                g = p * blocks + b
                out[p][b * 64 : b * 64 + 64, :] = total[g].astype(jnp.bfloat16)
                tile = jnp.zeros((8, 128), jnp.float32)
                for at, value in ((0, top[g]), (3, mass[g])):
                    for i in range(3):
                        part = value.astype(jnp.bfloat16).astype(jnp.float32)
                        tile = jnp.where(line == at + i, part, tile)
                        value = value - part
                stats.append(tile)
            out[p][blocks * 64 :, :] = jnp.concatenate(stats, axis=0).astype(jnp.bfloat16)


def attend(table, begin, q, kv, carry, last):
    rows = q[0].shape[0]
    blocks = rows // BLOCK
    groups = Y * blocks
    state = [jax.ShapeDtypeStruct((groups, BLOCK + 16, 128), jnp.float32)]
    if last:
        outs = [jax.ShapeDtypeStruct((rows + 8 * blocks, 128), jnp.bfloat16)] * Y
        scratch = [VMEM(s.shape, s.dtype) for s in state]
    else:
        outs, scratch = state, []
    outs = [VMEM(s.shape, s.dtype) for s in outs]
    args = [table] + [vmem(a) for a in (*q, *kv, *carry)]
    return pl.pallas_call(
        functools.partial(attend_kernel, blocks, len(kv), begin, last),
        out_shape=tuple(outs),
        in_specs=[full(SMEM)] + [full()] * (len(args) - 1),
        out_specs=(full(),) * len(outs),
        scratch_shapes=scratch,
        name="attend_late" if last else "attend_early",
        compiler_params=PARAMS,
    )(*args)


def merge_kernel(blocks, *refs):
    parts, out = refs[:-1], refs[-1]
    stats = [part[blocks * 64 :, :].astype(jnp.float32) for part in parts]
    for b in range(blocks):
        tops, masses = [], []
        for s in stats:
            t = s[b * 8 : b * 8 + 8]
            tops.append(t[0:1] + t[1:2] + t[2:3])
            masses.append(t[3:4] + t[4:5] + t[5:6])
        highest = functools.reduce(jnp.maximum, tops)
        mass, blended = 0.0, 0.0
        for part, m, l in zip(parts, tops, masses):
            scale = jnp.exp(m - highest)
            mass = mass + l * scale
            blended = blended + part[b * 64 : b * 64 + 64, :].astype(jnp.float32) * scale
        out[b * 64 : b * 64 + 64, :] = head_unturn(blended / mass).astype(jnp.bfloat16)


def merge(parts, blocks):
    return pl.pallas_call(
        functools.partial(merge_kernel, blocks),
        out_shape=VMEM((blocks * BLOCK, 128), jnp.bfloat16),
        in_specs=[full()] * len(parts),
        out_specs=full(),
        name="merge",
        compiler_params=PARAMS,
    )(*[vmem(a) for a in parts])


def finish_kernel(a0, a1, a2, a3, w0, w1, w2, w3, out):
    squares, summed = None, None
    for a, w in ((a0, w0), (a1, w1), (a2, w2), (a3, w3)):
        rows = a[...]
        wide = rows.astype(jnp.float32)
        term = jnp.dot(rows, w[...], preferred_element_type=jnp.float32)
        squares = wide * wide if squares is None else squares + wide * wide
        summed = term if summed is None else summed + term
    mean_sq = jnp.sum(squares, axis=1, keepdims=True) / (HEADS * HEAD_SIZE)
    out[...] = (summed * lax.rsqrt(mean_sq + eps_norm)).astype(jnp.bfloat16)


def finish(pieces, weights):
    rows, cols = pieces[0].shape[0], weights[0].shape[1]
    return pl.pallas_call(
        finish_kernel,
        out_shape=jax.ShapeDtypeStruct((rows, cols), jnp.bfloat16),
        in_specs=[full()] * 8,
        out_specs=full(),
        name="finish",
        compiler_params=PARAMS,
    )(*[vmem(a) for a in (*pieces, *weights)])


def on_device(
    tokens,
    query_weight,
    key_weight,
    value_weight,
    out_weight,
    norm_gain,
    chosen_owner,
    chosen_local,
):
    rows = tokens.shape[0]
    blocks = rows // BLOCK
    x, z, y, c = (lax.axis_index(name) for name in ("x", "z", "y", "c"))

    pieces = [tokens] + [lax.ppermute(tokens, "x", shift(X, s)) for s in (1, 2, 3)]
    at = jnp.stack([(x - s) % X for s in range(X)]).astype(jnp.int32)

    picked = chosen_owner * 8 + chosen_local
    picks = [picked] + [lax.ppermute(picked, "y", shift(Y, s)) for s in (1, 2, 3)]

    width = out_weight.shape[1] // X
    gained = []
    for s in range(X):
        columns = lax.dynamic_slice_in_dim(out_weight, ((x + s) % X) * width, width, 1)
        gained.append((columns.astype(jnp.float32) * norm_gain[:, None]).astype(jnp.bfloat16))
    weights = [gained[0]] + [lax.ppermute(gained[s], "x", shift(X, s)) for s in (1, 2, 3)]

    staged, weight = stage(tokens, (query_weight, key_weight, value_weight))
    q, kv = project(at, [staged] + pieces[1:], weight)

    places = [(i, j) for i in range(Z) for j in range(C)]

    def onward(k):
        return [(C * i + j, C * ((i + (k if j == 0 else -k)) % Z) + j) for i, j in places]

    def swap(a):
        return lax.ppermute(a, "c", [(0, 1), (1, 0)])

    same, cross = [kv], [swap(kv)]
    held = [(0, 0, kv), (0, 1, cross[0])]
    for step in (1, 2, 3):
        same.append(lax.ppermute(same[-1], ("z", "c"), onward(1)))
        cross.append(lax.ppermute(cross[-1], ("z", "c"), onward(1)))
        held += [(step, 0, same[-1]), (step, 1, cross[-1])]
        held += [(-step, 1, swap(same[-1])), (-step, 0, swap(cross[-1]))]
    far = lax.ppermute(same[2], ("z", "c"), onward(2))
    held += [(4, 0, far), (4, 1, swap(far))]

    queries = [q] + [lax.ppermute(q, "y", shift(Y, s)) for s in (1, 2, 3)]

    toward = 2 * c - 1
    column = jnp.stack(
        [((z + toward * d) % Z) * (Y * C) + y * C + (c ^ cc) for d, cc, _ in held]
    ).astype(jnp.int32)
    picks = jnp.stack(picks).reshape(Y, 1, -1)
    chosen = chosen_owner.shape[1]
    row = jnp.arange(blocks * chosen, dtype=jnp.int32) // chosen
    code = 1 + 8 * row + (picks & 7)
    hit = (picks >> 3) == column[None, :, None]
    table = jnp.sum(jnp.where(hit, code, 0), axis=2).reshape(-1)

    early = 10
    arrays = [a for _, _, a in held]
    carry = attend(table, 0, queries, arrays[:early], (), False)
    parts = attend(table, early, queries, arrays[early:], carry, True)

    back = [parts[0]] + [lax.ppermute(parts[s], "y", shift(Y, -s)) for s in (1, 2, 3)]
    attended = merge(back, blocks)
    spread = [attended] + [lax.ppermute(attended, "x", shift(X, s)) for s in (1, 2, 3)]
    return finish(spread, weights)


def solution(mesh):
    fine = Mesh(mesh.devices.reshape(Z, Y, C, X), ("z", "y", "c", "x"))
    kv = ("z", "y", "c")
    return jax.shard_map(
        on_device,
        mesh=fine,
        in_specs=(
            P(kv, "x"),
            P(None, "x"),
            P(None, "x"),
            P(None, "x"),
            P("x", None),
            P("x"),
            P(kv, None),
            P(kv, None),
        ),
        out_specs=P(kv, "x"),
        check_vma=False,
    )
```

```python
import functools

import jax
import jax.numpy as jnp
from jax import lax
from jax.experimental import pallas as pl
from jax.experimental.pallas import tpu as pltpu
from jax.sharding import Mesh
from jax.sharding import PartitionSpec as P

HEADS = 8
HEAD_SIZE = 64
BLOCK = 64
Z, Y, C, X = 8, 4, 2, 4

lowest = -1e30
eps_norm = 1e-06
VMEM = pltpu.VMEM
SMEM = pltpu.SMEM


PARAMS = pltpu.CompilerParams(vmem_limit_bytes=16 * 1024 * 1024)


def vmem(a):
    return pltpu.with_memory_space_constraint(a, VMEM)


def shift(n, s):
    return [(i, (i + s) % n) for i in range(n)]


def full(space=VMEM):
    return pl.BlockSpec(memory_space=space)


def head_turn(rows):
    turned = rows.T
    return jnp.concatenate([turned[:HEAD_SIZE], turned[HEAD_SIZE:]], axis=1)


def head_unturn(rows):
    return jnp.concatenate([rows[:, :HEAD_SIZE], rows[:, HEAD_SIZE:]], axis=0).T


def stage_kernel(tokens, wq, wk, wv, tokens_out, w_out):
    tokens_out[...] = tokens[...]
    for i, ref in enumerate((wq, wk, wv)):
        w_out[:, i * 128 : i * 128 + 128] = ref[...]


def stage(tokens, weights):
    depth, width = weights[0].shape
    return pl.pallas_call(
        stage_kernel,
        out_shape=(
            VMEM(tokens.shape, tokens.dtype),
            VMEM((depth, 3 * width), jnp.bfloat16),
        ),
        in_specs=[full()] * 4,
        out_specs=(full(),) * 2,
        name="stage",
        compiler_params=PARAMS,
    )(*[pltpu.with_memory_space_constraint(a, pltpu.HBM) for a in (tokens, *weights)])


def summed(at, pieces, weight, columns):
    total = None
    for s, piece in enumerate(pieces):
        rows = pl.ds(pl.multiple_of(at[s] * 256, 256), 256)
        term = jnp.dot(piece[...], weight[rows, columns], preferred_element_type=jnp.float32)
        total = term if total is None else total + term
    return total


def project_kernel(blocks, at, t0, t1, t2, t3, weight, kv_out):
    total = summed(at, (t0, t1, t2, t3), weight, slice(128, 384))
    half = blocks * BLOCK
    kv_out[:half, :] = total[:, :128].astype(jnp.bfloat16)
    for b in range(blocks):
        turned = head_turn(total[b * 64 : b * 64 + 64, 128:])
        kv_out[half + b * 64 : half + b * 64 + 64, :] = turned.astype(jnp.bfloat16)


def query_kernel(blocks, at, t0, t1, t2, t3, weight, picks, q_out):
    total = summed(at, (t0, t1, t2, t3), weight, slice(0, 128))
    total = total.astype(jnp.bfloat16).astype(jnp.float32) * (HEAD_SIZE ** (-0.5))
    for b in range(blocks):
        here = slice(b * 64, b * 64 + 64)
        q_out[here, :] = head_turn(total[here]).astype(jnp.bfloat16)
    q_out[blocks * BLOCK :, :] = picks[...]


def project(kernel, rows, at, *arrays):
    blocks = arrays[0].shape[0] // BLOCK
    return pl.pallas_call(
        functools.partial(kernel, blocks),
        out_shape=VMEM((rows, 128), jnp.bfloat16),
        in_specs=[full(SMEM)] + [full()] * len(arrays),
        out_specs=full(),
        compiler_params=PARAMS,
    )(at, *[vmem(a) for a in arrays])


def spread_heads(rows, lane):
    none = jnp.zeros_like(rows)
    return jnp.concatenate(
        [jnp.where(lane < HEAD_SIZE, rows, none), jnp.where(lane < HEAD_SIZE, none, rows)], axis=0
    )


def one_pair(q, k, v, lane, mask=None):
    scores = jnp.dot(k, spread_heads(q, lane), preferred_element_type=jnp.float32)
    if mask is not None:
        scores = jnp.where(mask, scores, lowest)
    highest = jnp.max(scores, axis=0, keepdims=True)
    weights = jnp.exp(scores - highest)
    mass = jnp.sum(weights, axis=0, keepdims=True)
    blended = jnp.dot(
        v, spread_heads(weights.astype(jnp.bfloat16), lane), preferred_element_type=jnp.float32
    )
    return highest, mass, blended


def attend_kernel(blocks, owners, begin, last, *refs):
    refs = list(refs)
    first = begin == 0
    table = refs.pop(0)
    q = [refs.pop(0) for _ in range(Y)]
    kv = [refs.pop(0) for _ in range(owners)]
    half = blocks * BLOCK
    carry = None if first else refs.pop(0)
    if last:
        out = [refs.pop(0) for _ in range(Y)]
    (state,) = refs
    total, top, mass = (state.at[:, a:b, :] for a, b in ((0, 64), (64, 72), (72, 80)))
    lane = lax.broadcasted_iota(jnp.int32, (BLOCK, 128), 1)

    if first:
        for g in range(blocks, Y * blocks):
            top[g] = jnp.full((8, 128), lowest, jnp.float32)
            mass[g] = jnp.zeros((8, 128), jnp.float32)
            total[g] = jnp.zeros((BLOCK, 128), jnp.float32)
        spot = lax.broadcasted_iota(jnp.int32, (BLOCK, 128), 0)
        seen = spot <= (lane & (HEAD_SIZE - 1))
        for b in range(blocks):
            here = slice(b * 64, b * 64 + 64)
            after = slice(half + b * 64, half + b * 64 + 64)
            m, l, o = one_pair(q[0][here, :], kv[0][here, :], kv[0][after, :], lane, seen)
            top[b] = jnp.broadcast_to(m, (8, 128))
            mass[b] = jnp.broadcast_to(l, (8, 128))
            total[b] = o
    else:
        state[...] = carry[...]

    for owner in range(owners):
        found = []
        for p in range(Y):
            code = table[p * (Z * C) + begin + owner]
            row = jnp.maximum(code - 1, 0)
            local = pl.multiple_of((row & 7) * BLOCK, BLOCK)
            row = row >> 3
            m, l, o = one_pair(
                q[p][pl.ds(pl.multiple_of(row * BLOCK, BLOCK), BLOCK), :],
                kv[owner][pl.ds(local, BLOCK), :],
                kv[owner][pl.ds(half + local, BLOCK), :],
                lane,
            )
            found.append((code > 0, p * blocks + row, m, l, o))
        for real, g, m, l, o in found:
            m = jnp.where(real, m, lowest)
            before = top[g]
            now = jnp.maximum(before, m)
            keep = jnp.exp(before - now)
            add = jnp.where(real, jnp.exp(m - now), 0.0)
            top[g] = now
            mass[g] = mass[g] * keep + l * add
            total[g] = total[g] * keep[:1] + o * add[:1]

    if last:
        line = lax.broadcasted_iota(jnp.int32, (8, 128), 0)
        for p in range(Y):
            stats = []
            for b in range(blocks):
                g = p * blocks + b
                out[p][b * 64 : b * 64 + 64, :] = total[g].astype(jnp.bfloat16)
                tile = jnp.zeros((8, 128), jnp.float32)
                for at, value in ((0, top[g]), (3, mass[g])):
                    for i in range(3):
                        part = value.astype(jnp.bfloat16).astype(jnp.float32)
                        tile = jnp.where(line == at + i, part, tile)
                        value = value - part
                stats.append(tile)
            out[p][blocks * 64 :, :] = jnp.concatenate(stats, axis=0).astype(jnp.bfloat16)


def attend(table, begin, q, kv, carry, last, blocks):
    rows = blocks * BLOCK
    state = VMEM((Y * blocks, BLOCK + 16, 128), jnp.float32)
    outs = [VMEM((rows + 8 * blocks, 128), jnp.bfloat16)] * Y if last else [state]
    args = [table] + [vmem(a) for a in (*q, *kv, *carry)]
    return pl.pallas_call(
        functools.partial(attend_kernel, blocks, len(kv), begin, last),
        out_shape=tuple(outs),
        in_specs=[full(SMEM)] + [full()] * (len(args) - 1),
        out_specs=(full(),) * len(outs),
        scratch_shapes=[state] if last else [],
        compiler_params=PARAMS,
    )(*args)


def merge_kernel(blocks, *refs):
    parts, out = refs[:-1], refs[-1]
    stats = [part[blocks * 64 :, :].astype(jnp.float32) for part in parts]
    for b in range(blocks):
        tops, masses = [], []
        for s in stats:
            t = s[b * 8 : b * 8 + 8]
            tops.append(t[0:1] + t[1:2] + t[2:3])
            masses.append(t[3:4] + t[4:5] + t[5:6])
        highest = functools.reduce(jnp.maximum, tops)
        mass, blended = 0.0, 0.0
        for part, m, l in zip(parts, tops, masses):
            scale = jnp.exp(m - highest)
            mass = mass + l * scale
            blended = blended + part[b * 64 : b * 64 + 64, :].astype(jnp.float32) * scale
        out[b * 64 : b * 64 + 64, :] = head_unturn(blended / mass).astype(jnp.bfloat16)


def merge(parts, blocks):
    return pl.pallas_call(
        functools.partial(merge_kernel, blocks),
        out_shape=VMEM((blocks * BLOCK, 128), jnp.bfloat16),
        in_specs=[full()] * len(parts),
        out_specs=full(),
        name="merge",
        compiler_params=PARAMS,
    )(*[vmem(a) for a in parts])


def finish_kernel(a0, a1, a2, a3, w0, w1, w2, w3, out):
    squares, summed = None, None
    for a, w in ((a0, w0), (a1, w1), (a2, w2), (a3, w3)):
        rows = a[...]
        wide = rows.astype(jnp.float32)
        term = jnp.dot(rows, w[...], preferred_element_type=jnp.float32)
        squares = wide * wide if squares is None else squares + wide * wide
        summed = term if summed is None else summed + term
    mean_sq = jnp.sum(squares, axis=1, keepdims=True) / (HEADS * HEAD_SIZE)
    out[...] = (summed * lax.rsqrt(mean_sq + eps_norm)).astype(jnp.bfloat16)


def finish(pieces, weights):
    rows, cols = pieces[0].shape[0], weights[0].shape[1]
    return pl.pallas_call(
        finish_kernel,
        out_shape=jax.ShapeDtypeStruct((rows, cols), jnp.bfloat16),
        in_specs=[full()] * 8,
        out_specs=full(),
        name="finish",
        compiler_params=PARAMS,
    )(*[vmem(a) for a in (*pieces, *weights)])


def on_device(
    tokens,
    query_weight,
    key_weight,
    value_weight,
    out_weight,
    norm_gain,
    chosen_owner,
    chosen_local,
):
    rows = tokens.shape[0]
    blocks = rows // BLOCK
    x, z, y, c = (lax.axis_index(name) for name in ("x", "z", "y", "c"))

    pieces = [tokens] + [lax.ppermute(tokens, "x", shift(X, s)) for s in (1, 2, 3)]
    at = jnp.stack([(x - s) % X for s in range(X)]).astype(jnp.int32)

    width = out_weight.shape[1] // X
    gained = []
    for s in range(X):
        columns = lax.dynamic_slice_in_dim(out_weight, ((x + s) % X) * width, width, 1)
        gained.append((columns.astype(jnp.float32) * norm_gain[:, None]).astype(jnp.bfloat16))
    weights = [gained[0]] + [lax.ppermute(gained[s], "x", shift(X, s)) for s in (1, 2, 3)]

    staged, weight = stage(tokens, (query_weight, key_weight, value_weight))
    pieces[0] = staged
    kv = project(project_kernel, 2 * rows, at, *pieces, weight)
    chosen = jnp.stack([chosen_owner.reshape(-1), chosen_local.reshape(-1)])
    count = chosen.shape[1]
    chosen = jnp.pad(chosen.astype(jnp.bfloat16), ((0, 14), (0, 128 - count)))
    q = project(query_kernel, rows + 16, at, *pieces, weight, chosen)

    places = [(i, j) for i in range(Z) for j in range(C)]

    def onward(k):
        return [(C * i + j, C * ((i + (k if j == 0 else -k)) % Z) + j) for i, j in places]

    def swap(a):
        return lax.ppermute(a, "c", [(0, 1), (1, 0)])

    same, cross = [kv], [swap(kv)]
    held = [(0, 0, kv), (0, 1, cross[0])]
    for step in (1, 2, 3):
        reach = (0, 1, 2, 1)[step]
        same.append(lax.ppermute(same[step - reach], ("z", "c"), onward(reach)))
        cross.append(lax.ppermute(cross[step - reach], ("z", "c"), onward(reach)))
        held += [(step, 0, same[-1]), (-step, 1, swap(same[-1]))]
        held += [(step, 1, cross[-1]), (-step, 0, swap(cross[-1]))]
    far = lax.ppermute(same[2], ("z", "c"), onward(2))
    held += [(4, 0, far), (4, 1, swap(far))]

    queries = [q] + [lax.ppermute(q, "y", shift(Y, s)) for s in (1, 2, 3)]

    toward = 2 * c - 1
    column = jnp.stack(
        [((z + toward * d) % Z) * (Y * C) + y * C + (c ^ cc) for d, cc, _ in held]
    ).astype(jnp.int32)
    picks = [a[rows:].astype(jnp.float32).astype(jnp.int32) for a in queries]
    owner = jnp.stack([a[0, :count] for a in picks])[:, None, :]
    local = jnp.stack([a[1, :count] for a in picks])[:, None, :]
    row = jnp.arange(count, dtype=jnp.int32) // chosen_owner.shape[1]
    hit = owner == column[None, :, None]
    table = jnp.sum(jnp.where(hit, 1 + 8 * row + local, 0), axis=2).reshape(-1)

    arrays = [a for _, _, a in held]
    carry, begin = (), 0
    for name, end in (("early", 10), ("middle", 12), ("late", Z * C)):
        parts = attend(table, begin, queries, arrays[begin:end], carry, name == "late", blocks)
        carry, begin = parts[-1:], end

    back = [parts[0]] + [lax.ppermute(parts[s], "y", shift(Y, -s)) for s in (1, 2, 3)]
    attended = merge(back, blocks)
    spread = [attended] + [lax.ppermute(attended, "x", shift(X, s)) for s in (1, 2, 3)]
    return finish(spread, weights)


def solution(mesh):
    fine = Mesh(mesh.devices.reshape(Z, Y, C, X), ("z", "y", "c", "x"))
    kv = ("z", "y", "c")
    return jax.shard_map(
        on_device,
        mesh=fine,
        in_specs=(
            P(kv, "x"),
            P(None, "x"),
            P(None, "x"),
            P(None, "x"),
            P("x", None),
            P("x"),
            P(kv, None),
            P(kv, None),
        ),
        out_specs=P(kv, "x"),
        check_vma=False,
    )
```

```python
import functools

import jax
import jax.numpy as jnp
from jax import lax
from jax.experimental import pallas as pl
from jax.experimental.pallas import tpu as pltpu
from jax.sharding import Mesh
from jax.sharding import PartitionSpec as P

HEADS = 8
HEAD_SIZE = 64
BLOCK = 64
Z, Y, C, X = 8, 4, 2, 4

lowest = -1e30
eps_norm = 1e-06
VMEM = pltpu.VMEM


PARAMS = pltpu.CompilerParams(vmem_limit_bytes=16 * 1024 * 1024)


def vmem(a):
    return pltpu.with_memory_space_constraint(a, VMEM)


def shift(n, s):
    return [(i, (i + s) % n) for i in range(n)]


def full(space=VMEM):
    return pl.BlockSpec(memory_space=space)


def head_turn(rows):
    turned = rows.T
    return jnp.concatenate([turned[:HEAD_SIZE], turned[HEAD_SIZE:]], axis=1)


def head_unturn(rows):
    return jnp.concatenate([rows[:, :HEAD_SIZE], rows[:, HEAD_SIZE:]], axis=0).T


def stage_kernel(tokens, wq, wk, wv, w_out, total_out):
    for i, ref in enumerate((wq, wk, wv)):
        w_out[:, i * 128 : i * 128 + 128] = ref[...]
    total_out[...] = term_of(0, tokens, w_out, slice(0, 384))


def stage(tokens, weights):
    depth, width = weights[0].shape
    arrays = [pltpu.with_memory_space_constraint(a, pltpu.HBM) for a in (tokens, *weights)]
    return pl.pallas_call(
        stage_kernel,
        out_shape=(
            VMEM((depth, 3 * width), jnp.bfloat16),
            VMEM((tokens.shape[0], 3 * width), jnp.float32),
        ),
        in_specs=[full()] * 4,
        out_specs=(full(),) * 2,
        name="stage",
        compiler_params=PARAMS,
    )(*arrays)


def term_of(back, piece, weight, columns):
    place = (lax.axis_index("x") + (X - back)) & (X - 1)
    depth = piece.shape[1]
    rows = pl.ds(pl.multiple_of(place * depth, depth), depth)
    return jnp.dot(piece[...], weight[rows, columns], preferred_element_type=jnp.float32)


def summed(total, pieces, weight, columns):
    total = total[:, columns]
    for s, piece in enumerate(pieces, 1):
        total = total + term_of(s, piece, weight, columns)
    return total


def project_kernel(blocks, t0, t1, t2, t3, weight, kv_out):
    total = summed(t0, (t1, t2, t3), weight, slice(128, 384))
    half = blocks * BLOCK
    kv_out[:half, :] = total[:, :128].astype(jnp.bfloat16)
    for b in range(blocks):
        turned = head_turn(total[b * 64 : b * 64 + 64, 128:])
        kv_out[half + b * 64 : half + b * 64 + 64, :] = turned.astype(jnp.bfloat16)


def query_kernel(blocks, t0, t1, t2, t3, weight, picks, q_out):
    total = summed(t0, (t1, t2, t3), weight, slice(0, 128))
    total = total.astype(jnp.bfloat16).astype(jnp.float32) * (HEAD_SIZE ** (-0.5))
    for b in range(blocks):
        here = slice(b * 64, b * 64 + 64)
        q_out[here, :] = head_turn(total[here]).astype(jnp.bfloat16)
    q_out[blocks * BLOCK :, :] = picks[...]


def project(kernel, rows, *arrays):
    blocks = arrays[0].shape[0] // BLOCK
    return pl.pallas_call(
        functools.partial(kernel, blocks),
        out_shape=VMEM((rows, 128), jnp.bfloat16),
        in_specs=[full()] * len(arrays),
        out_specs=full(),
        compiler_params=PARAMS,
    )(*[vmem(a) for a in arrays])


def spread_heads(rows, lane):
    none = jnp.zeros_like(rows)
    return jnp.concatenate(
        [jnp.where(lane < HEAD_SIZE, rows, none), jnp.where(lane < HEAD_SIZE, none, rows)], axis=0
    )


def one_pair(q, k, v, lane, mask=None):
    scores = jnp.dot(k, spread_heads(q, lane), preferred_element_type=jnp.float32)
    if mask is not None:
        scores = jnp.where(mask, scores, lowest)
    highest = jnp.max(scores, axis=0, keepdims=True)
    weights = jnp.exp(scores - highest)
    mass = jnp.sum(weights, axis=0, keepdims=True)
    blended = jnp.dot(
        v, spread_heads(weights.astype(jnp.bfloat16), lane), preferred_element_type=jnp.float32
    )
    return highest, mass, blended


def attend_kernel(blocks, owners, begin, last, *refs):
    refs = list(refs)
    first = begin == 0
    table = refs.pop(0)[...]
    q = [refs.pop(0) for _ in range(Y)]
    kv = [refs.pop(0) for _ in range(owners)]
    half = blocks * BLOCK
    carry = None if first else refs.pop(0)
    if last:
        out = [refs.pop(0) for _ in range(Y)]
    (state,) = refs
    total, top, mass = (state.at[:, a:b, :] for a, b in ((0, 64), (64, 72), (72, 80)))
    lane = lax.broadcasted_iota(jnp.int32, (BLOCK, 128), 1)

    if first:
        for g in range(blocks, Y * blocks):
            top[g] = jnp.full((8, 128), lowest, jnp.float32)
            mass[g] = jnp.zeros((8, 128), jnp.float32)
            total[g] = jnp.zeros((BLOCK, 128), jnp.float32)
        spot = lax.broadcasted_iota(jnp.int32, (BLOCK, 128), 0)
        seen = spot <= (lane & (HEAD_SIZE - 1))
        for b in range(blocks):
            here = slice(b * 64, b * 64 + 64)
            after = slice(half + b * 64, half + b * 64 + 64)
            m, l, o = one_pair(q[0][here, :], kv[0][here, :], kv[0][after, :], lane, seen)
            top[b] = jnp.broadcast_to(m, (8, 128))
            mass[b] = jnp.broadcast_to(l, (8, 128))
            total[b] = o
    else:
        state[...] = carry[...]

    for owner in range(owners):
        found = []
        for p in range(Y):
            code = table[p, begin + owner]
            row = jnp.maximum(code - 1, 0)
            local = pl.multiple_of((row & 7) * BLOCK, BLOCK)
            row = row >> 3
            m, l, o = one_pair(
                q[p][pl.ds(pl.multiple_of(row * BLOCK, BLOCK), BLOCK), :],
                kv[owner][pl.ds(local, BLOCK), :],
                kv[owner][pl.ds(half + local, BLOCK), :],
                lane,
            )
            found.append((code > 0, p * blocks + row, m, l, o))
        for real, g, m, l, o in found:
            m = jnp.where(real, m, lowest)
            before = top[g]
            now = jnp.maximum(before, m)
            keep = jnp.exp(before - now)
            add = jnp.where(real, jnp.exp(m - now), 0.0)
            top[g] = now
            mass[g] = mass[g] * keep + l * add
            total[g] = total[g] * keep[:1] + o * add[:1]

    if last:
        line = lax.broadcasted_iota(jnp.int32, (8, 128), 0)
        for p in range(Y):
            stats = []
            for b in range(blocks):
                g = p * blocks + b
                out[p][b * 64 : b * 64 + 64, :] = total[g].astype(jnp.bfloat16)
                tile = jnp.zeros((8, 128), jnp.float32)
                for at, value in ((0, top[g]), (3, mass[g])):
                    for i in range(3):
                        part = value.astype(jnp.bfloat16).astype(jnp.float32)
                        tile = jnp.where(line == at + i, part, tile)
                        value = value - part
                stats.append(tile)
            out[p][blocks * 64 :, :] = jnp.concatenate(stats, axis=0).astype(jnp.bfloat16)


def attend(table, begin, q, kv, carry, last, blocks):
    rows = blocks * BLOCK
    state = VMEM((Y * blocks, BLOCK + 16, 128), jnp.float32)
    outs = [VMEM((rows + 8 * blocks, 128), jnp.bfloat16)] * Y if last else [state]
    args = [vmem(a) for a in (table, *q, *kv, *carry)]
    return pl.pallas_call(
        functools.partial(attend_kernel, blocks, len(kv), begin, last),
        out_shape=tuple(outs),
        in_specs=[full()] * len(args),
        out_specs=(full(),) * len(outs),
        scratch_shapes=[state] if last else [],
        compiler_params=PARAMS,
    )(*args)


def merge_kernel(blocks, *refs):
    parts, out = refs[:-1], refs[-1]
    stats = [part[blocks * 64 :, :].astype(jnp.float32) for part in parts]
    for b in range(blocks):
        tops, masses = [], []
        for s in stats:
            t = s[b * 8 : b * 8 + 8]
            tops.append(t[0:1] + t[1:2] + t[2:3])
            masses.append(t[3:4] + t[4:5] + t[5:6])
        highest = functools.reduce(jnp.maximum, tops)
        mass, blended = 0.0, 0.0
        for part, m, l in zip(parts, tops, masses):
            scale = jnp.exp(m - highest)
            mass = mass + l * scale
            blended = blended + part[b * 64 : b * 64 + 64, :].astype(jnp.float32) * scale
        out[b * 64 : b * 64 + 64, :] = head_unturn(blended / mass).astype(jnp.bfloat16)


def merge(parts, blocks):
    return pl.pallas_call(
        functools.partial(merge_kernel, blocks),
        out_shape=VMEM((blocks * BLOCK, 128), jnp.bfloat16),
        in_specs=[full()] * len(parts),
        out_specs=full(),
        name="merge",
        compiler_params=PARAMS,
    )(*[vmem(a) for a in parts])


def finish_kernel(a0, a1, a2, a3, w0, w1, w2, w3, out):
    squares, summed = None, None
    for a, w in ((a0, w0), (a1, w1), (a2, w2), (a3, w3)):
        rows = a[...]
        wide = rows.astype(jnp.float32)
        term = jnp.dot(rows, w[...], preferred_element_type=jnp.float32)
        squares = wide * wide if squares is None else squares + wide * wide
        summed = term if summed is None else summed + term
    mean_sq = jnp.sum(squares, axis=1, keepdims=True) / (HEADS * HEAD_SIZE)
    out[...] = (summed * lax.rsqrt(mean_sq + eps_norm)).astype(jnp.bfloat16)


def finish(pieces, weights):
    rows, cols = pieces[0].shape[0], weights[0].shape[1]
    return pl.pallas_call(
        finish_kernel,
        out_shape=jax.ShapeDtypeStruct((rows, cols), jnp.bfloat16),
        in_specs=[full()] * 8,
        out_specs=full(),
        name="finish",
        compiler_params=PARAMS,
    )(*[vmem(a) for a in (*pieces, *weights)])


def on_device(
    tokens,
    query_weight,
    key_weight,
    value_weight,
    out_weight,
    norm_gain,
    chosen_owner,
    chosen_local,
):
    rows = tokens.shape[0]
    blocks = rows // BLOCK
    x, z, y, c = (lax.axis_index(name) for name in ("x", "z", "y", "c"))

    pieces = [tokens] + [lax.ppermute(tokens, "x", shift(X, s)) for s in (1, 2, 3)]

    width = out_weight.shape[1] // X
    gained = []
    for s in range(X):
        columns = lax.dynamic_slice_in_dim(out_weight, ((x + s) % X) * width, width, 1)
        gained.append((columns.astype(jnp.float32) * norm_gain[:, None]).astype(jnp.bfloat16))
    weights = [gained[0]] + [lax.ppermute(gained[s], "x", shift(X, s)) for s in (1, 2, 3)]

    weight, pieces[0] = stage(tokens, (query_weight, key_weight, value_weight))
    kv = project(project_kernel, 2 * rows, *pieces, weight)
    chosen = jnp.stack([chosen_owner.reshape(-1), chosen_local.reshape(-1)])
    count = chosen.shape[1]
    chosen = jnp.pad(chosen.astype(jnp.bfloat16), ((0, 14), (0, 128 - count)))
    q = project(query_kernel, rows + 16, *pieces, weight, chosen)

    places = [(i, j) for i in range(Z) for j in range(C)]

    def onward(k):
        return [(C * i + j, C * ((i + (k if j == 0 else -k)) % Z) + j) for i, j in places]

    def swap(a):
        return lax.ppermute(a, "c", [(0, 1), (1, 0)])

    same, cross = [kv], [swap(kv)]
    held = [(0, 0, kv), (0, 1, cross[0])]
    for step in (1, 2, 3):
        reach = (0, 1, 2, 1)[step]
        same.append(lax.ppermute(same[step - reach], ("z", "c"), onward(reach)))
        cross.append(lax.ppermute(cross[step - reach], ("z", "c"), onward(reach)))
        held += [(step, 0, same[-1]), (-step, 1, swap(same[-1]))]
        held += [(step, 1, cross[-1]), (-step, 0, swap(cross[-1]))]
    far = lax.ppermute(same[2], ("z", "c"), onward(2))
    held += [(4, 0, far), (4, 1, swap(far))]
    held[13], held[14] = held[14], held[13]

    queries = [q] + [lax.ppermute(q, "y", shift(Y, s)) for s in (1, 2, 3)]

    toward = 2 * c - 1
    column = jnp.stack(
        [((z + toward * d) % Z) * (Y * C) + y * C + (c ^ cc) for d, cc, _ in held]
    ).astype(jnp.int32)
    picks = [a[rows:].astype(jnp.float32).astype(jnp.int32) for a in queries]
    owner = jnp.stack([a[0, :count] for a in picks])[:, None, :]
    local = jnp.stack([a[1, :count] for a in picks])[:, None, :]
    row = jnp.arange(count, dtype=jnp.int32) // chosen_owner.shape[1]
    hit = owner == column[None, :, None]
    table = jnp.sum(jnp.where(hit, 1 + 8 * row + local, 0), axis=2)

    arrays = [a for _, _, a in held]
    carry, begin = (), 0
    for name, end in (("early", 10), ("middle", 12), ("nearly", 14), ("late", Z * C)):
        parts = attend(table, begin, queries, arrays[begin:end], carry, name == "late", blocks)
        carry, begin = parts[-1:], end

    back = [parts[0]] + [lax.ppermute(parts[s], "y", shift(Y, -s)) for s in (1, 2, 3)]
    attended = merge(back, blocks)
    spread = [attended] + [lax.ppermute(attended, "x", shift(X, s)) for s in (1, 2, 3)]
    return finish(spread, weights)


def solution(mesh):
    fine = Mesh(mesh.devices.reshape(Z, Y, C, X), ("z", "y", "c", "x"))
    kv = ("z", "y", "c")
    return jax.shard_map(
        on_device,
        mesh=fine,
        in_specs=(
            P(kv, "x"),
            P(None, "x"),
            P(None, "x"),
            P(None, "x"),
            P("x", None),
            P("x"),
            P(kv, None),
            P(kv, None),
        ),
        out_specs=P(kv, "x"),
        check_vma=False,
    )
```

```python
import functools

import jax
import jax.numpy as jnp
from jax import lax
from jax.experimental import pallas as pl
from jax.experimental.pallas import tpu as pltpu
from jax.sharding import Mesh
from jax.sharding import PartitionSpec as P

HEADS = 8
HEAD_SIZE = 64
BLOCK = 64
Z, Y, C, X = 8, 4, 2, 4

lowest = -1e30
eps_norm = 1e-06
VMEM = pltpu.VMEM


PARAMS = pltpu.CompilerParams(vmem_limit_bytes=16 * 1024 * 1024)


def vmem(a):
    return pltpu.with_memory_space_constraint(a, VMEM)


def shift(n, s):
    return [(i, (i + s) % n) for i in range(n)]


def full(space=VMEM):
    return pl.BlockSpec(memory_space=space)


def head_turn(rows):
    turned = rows.T
    return jnp.concatenate([turned[:HEAD_SIZE], turned[HEAD_SIZE:]], axis=1)


def head_unturn(rows):
    return jnp.concatenate([rows[:, :HEAD_SIZE], rows[:, HEAD_SIZE:]], axis=0).T


def stage_kernel(tokens, wq, wk, wv, w_out, total_out):
    for i, ref in enumerate((wq, wk, wv)):
        w_out[:, i * 128 : i * 128 + 128] = ref[...]
    total_out[...] = term_of(0, tokens, w_out, slice(0, 384))


def stage(tokens, weights):
    depth, width = weights[0].shape
    arrays = [pltpu.with_memory_space_constraint(a, pltpu.HBM) for a in (tokens, *weights)]
    return pl.pallas_call(
        stage_kernel,
        out_shape=(
            VMEM((depth, 3 * width), jnp.bfloat16),
            VMEM((tokens.shape[0], 3 * width), jnp.float32),
        ),
        in_specs=[full()] * 4,
        out_specs=(full(),) * 2,
        name="stage",
        compiler_params=PARAMS,
    )(*arrays)


def term_of(back, piece, weight, columns):
    place = (lax.axis_index("x") + (X - back)) & (X - 1)
    depth = piece.shape[1]
    rows = pl.ds(pl.multiple_of(place * depth, depth), depth)
    return jnp.dot(piece[...], weight[rows, columns], preferred_element_type=jnp.float32)


def summed(total, pieces, weight, columns):
    total = total[:, columns]
    for s, piece in enumerate(pieces, 1):
        total = total + term_of(s, piece, weight, columns)
    return total


def project_kernel(blocks, t0, t1, t2, t3, weight, kv_out):
    total = summed(t0, (t1, t2, t3), weight, slice(128, 384))
    half = blocks * BLOCK
    kv_out[:half, :] = total[:, :128].astype(jnp.bfloat16)
    for b in range(blocks):
        turned = head_turn(total[b * 64 : b * 64 + 64, 128:])
        kv_out[half + b * 64 : half + b * 64 + 64, :] = turned.astype(jnp.bfloat16)


def query_kernel(blocks, t0, t1, t2, t3, weight, picks, q_out):
    total = summed(t0, (t1, t2, t3), weight, slice(0, 128))
    total = total.astype(jnp.bfloat16).astype(jnp.float32) * (HEAD_SIZE ** (-0.5))
    for b in range(blocks):
        here = slice(b * 64, b * 64 + 64)
        q_out[here, :] = head_turn(total[here]).astype(jnp.bfloat16)
    q_out[blocks * BLOCK :, :] = picks[...]


def project(kernel, rows, *arrays):
    blocks = arrays[0].shape[0] // BLOCK
    return pl.pallas_call(
        functools.partial(kernel, blocks),
        out_shape=VMEM((rows, 128), jnp.bfloat16),
        in_specs=[full()] * len(arrays),
        out_specs=full(),
        compiler_params=PARAMS,
    )(*[vmem(a) for a in arrays])


def spread_heads(rows, lane):
    none = jnp.zeros_like(rows)
    return jnp.concatenate(
        [jnp.where(lane < HEAD_SIZE, rows, none), jnp.where(lane < HEAD_SIZE, none, rows)], axis=0
    )


def one_pair(q, k, v, lane, mask=None):
    scores = jnp.dot(k, spread_heads(q, lane), preferred_element_type=jnp.float32)
    if mask is not None:
        scores = jnp.where(mask, scores, lowest)
    highest = jnp.max(scores, axis=0, keepdims=True)
    weights = jnp.exp(scores - highest)
    mass = jnp.sum(weights, axis=0, keepdims=True)
    blended = jnp.dot(
        v, spread_heads(weights.astype(jnp.bfloat16), lane), preferred_element_type=jnp.float32
    )
    return highest, mass, blended


def attend_kernel(blocks, owners, begin, last, *refs):
    refs = list(refs)
    first = begin == 0
    table = refs.pop(0)[...]
    q = [refs.pop(0) for _ in range(Y)]
    kv = [refs.pop(0) for _ in range(owners)]
    half = blocks * BLOCK
    carry = None if first else refs.pop(0)
    if last:
        out = [refs.pop(0) for _ in range(Y)]
    (state,) = refs
    total, top, mass = (state.at[:, a:b, :] for a, b in ((0, 64), (64, 72), (72, 80)))
    lane = lax.broadcasted_iota(jnp.int32, (BLOCK, 128), 1)

    if first:
        for g in range(blocks, Y * blocks):
            top[g] = jnp.full((8, 128), lowest, jnp.float32)
            mass[g] = jnp.zeros((8, 128), jnp.float32)
            total[g] = jnp.zeros((BLOCK, 128), jnp.float32)
        spot = lax.broadcasted_iota(jnp.int32, (BLOCK, 128), 0)
        seen = spot <= (lane & (HEAD_SIZE - 1))
        for b in range(blocks):
            here = slice(b * 64, b * 64 + 64)
            after = slice(half + b * 64, half + b * 64 + 64)
            m, l, o = one_pair(q[0][here, :], kv[0][here, :], kv[0][after, :], lane, seen)
            top[b] = jnp.broadcast_to(m, (8, 128))
            mass[b] = jnp.broadcast_to(l, (8, 128))
            total[b] = o
    else:
        state[...] = carry[...]

    for owner in range(owners):
        found = []
        for p in range(Y):
            code = table[p, begin + owner]
            row = jnp.maximum(code - 1, 0)
            local = pl.multiple_of((row & 7) * BLOCK, BLOCK)
            row = row >> 3
            m, l, o = one_pair(
                q[p][pl.ds(pl.multiple_of(row * BLOCK, BLOCK), BLOCK), :],
                kv[owner][pl.ds(local, BLOCK), :],
                kv[owner][pl.ds(half + local, BLOCK), :],
                lane,
            )
            found.append((code > 0, p * blocks + row, m, l, o))
        for real, g, m, l, o in found:
            m = jnp.where(real, m, lowest)
            before = top[g]
            now = jnp.maximum(before, m)
            keep = jnp.exp(before - now)
            add = jnp.where(real, jnp.exp(m - now), 0.0)
            top[g] = now
            mass[g] = mass[g] * keep + l * add
            total[g] = total[g] * keep[:1] + o * add[:1]

    if last:
        line = lax.broadcasted_iota(jnp.int32, (8, 128), 0)
        for p in range(Y):
            stats = []
            for b in range(blocks):
                g = p * blocks + b
                out[p][b * 64 : b * 64 + 64, :] = total[g].astype(jnp.bfloat16)
                tile = jnp.zeros((8, 128), jnp.float32)
                for at, value in ((0, top[g]), (3, mass[g])):
                    for i in range(3):
                        part = value.astype(jnp.bfloat16).astype(jnp.float32)
                        tile = jnp.where(line == at + i, part, tile)
                        value = value - part
                stats.append(tile)
            out[p][blocks * 64 :, :] = jnp.concatenate(stats, axis=0).astype(jnp.bfloat16)


def attend(table, begin, q, kv, carry, last, blocks):
    rows = blocks * BLOCK
    state = VMEM((Y * blocks, BLOCK + 16, 128), jnp.float32)
    outs = [VMEM((rows + 8 * blocks, 128), jnp.bfloat16)] * Y if last else [state]
    args = [vmem(a) for a in (table, *q, *kv, *carry)]
    return pl.pallas_call(
        functools.partial(attend_kernel, blocks, len(kv), begin, last),
        out_shape=tuple(outs),
        in_specs=[full()] * len(args),
        out_specs=(full(),) * len(outs),
        scratch_shapes=[state] if last else [],
        compiler_params=PARAMS,
    )(*args)


def merge_kernel(blocks, *refs):
    parts, out = refs[:-1], refs[-1]
    stats = [part[blocks * 64 :, :].astype(jnp.float32) for part in parts]
    for b in range(blocks):
        tops, masses = [], []
        for s in stats:
            t = s[b * 8 : b * 8 + 8]
            tops.append(t[0:1] + t[1:2] + t[2:3])
            masses.append(t[3:4] + t[4:5] + t[5:6])
        highest = functools.reduce(jnp.maximum, tops)
        mass, blended = 0.0, 0.0
        for part, m, l in zip(parts, tops, masses):
            scale = jnp.exp(m - highest)
            mass = mass + l * scale
            blended = blended + part[b * 64 : b * 64 + 64, :].astype(jnp.float32) * scale
        out[b * 64 : b * 64 + 64, :] = head_unturn(blended / mass).astype(jnp.bfloat16)


def merge(parts, blocks):
    return pl.pallas_call(
        functools.partial(merge_kernel, blocks),
        out_shape=VMEM((blocks * BLOCK, 128), jnp.bfloat16),
        in_specs=[full()] * len(parts),
        out_specs=full(),
        name="merge",
        compiler_params=PARAMS,
    )(*[vmem(a) for a in parts])


def begin_kernel(a, w, total, squares):
    rows = a[...]
    total[...] = jnp.dot(rows, w[...], preferred_element_type=jnp.float32)
    wide = rows.astype(jnp.float32)
    squares[...] = wide * wide


def open_output(piece, weight):
    rows, cols = piece.shape[0], weight.shape[1]
    return pl.pallas_call(
        begin_kernel,
        out_shape=(VMEM((rows, cols), jnp.float32), VMEM(piece.shape, jnp.float32)),
        in_specs=[full()] * 2,
        out_specs=(full(),) * 2,
        name="begin",
        compiler_params=PARAMS,
    )(vmem(piece), vmem(weight))


def finish_kernel(t, q, a1, a2, a3, w1, w2, w3, out):
    total, squares = t[...], q[...]
    for a, w in ((a1, w1), (a2, w2), (a3, w3)):
        rows = a[...]
        wide = rows.astype(jnp.float32)
        squares = squares + wide * wide
        total = total + jnp.dot(rows, w[...], preferred_element_type=jnp.float32)
    mean_sq = jnp.sum(squares, axis=1, keepdims=True) / (HEADS * HEAD_SIZE)
    out[...] = (total * lax.rsqrt(mean_sq + eps_norm)).astype(jnp.bfloat16)


def finish(started, pieces, weights):
    rows, cols = started[0].shape
    return pl.pallas_call(
        finish_kernel,
        out_shape=jax.ShapeDtypeStruct((rows, cols), jnp.bfloat16),
        in_specs=[full()] * 8,
        out_specs=full(),
        name="finish",
        compiler_params=PARAMS,
    )(*[vmem(a) for a in (*started, *pieces, *weights)])


def on_device(
    tokens,
    query_weight,
    key_weight,
    value_weight,
    out_weight,
    norm_gain,
    chosen_owner,
    chosen_local,
):
    rows = tokens.shape[0]
    blocks = rows // BLOCK
    x, z, y, c = (lax.axis_index(name) for name in ("x", "z", "y", "c"))

    pieces = [tokens] + [lax.ppermute(tokens, "x", shift(X, s)) for s in (1, 2, 3)]

    width = out_weight.shape[1] // X
    gained = []
    for s in range(X):
        columns = lax.dynamic_slice_in_dim(out_weight, ((x + s) % X) * width, width, 1)
        gained.append((columns.astype(jnp.float32) * norm_gain[:, None]).astype(jnp.bfloat16))
    weights = [gained[0]] + [lax.ppermute(gained[s], "x", shift(X, s)) for s in (1, 2, 3)]

    weight, pieces[0] = stage(tokens, (query_weight, key_weight, value_weight))
    kv = project(project_kernel, 2 * rows, *pieces, weight)
    chosen = jnp.stack([chosen_owner.reshape(-1), chosen_local.reshape(-1)])
    count = chosen.shape[1]
    chosen = jnp.pad(chosen.astype(jnp.bfloat16), ((0, 14), (0, 128 - count)))
    q = project(query_kernel, rows + 16, *pieces, weight, chosen)

    places = [(i, j) for i in range(Z) for j in range(C)]

    def onward(k):
        return [(C * i + j, C * ((i + (k if j == 0 else -k)) % Z) + j) for i, j in places]

    def swap(a):
        return lax.ppermute(a, "c", [(0, 1), (1, 0)])

    same, cross = [kv], [swap(kv)]
    held = [(0, 0, kv), (0, 1, cross[0])]
    for step in (1, 2, 3):
        reach = (0, 1, 2, 1)[step]
        same.append(lax.ppermute(same[step - reach], ("z", "c"), onward(reach)))
        cross.append(lax.ppermute(cross[step - reach], ("z", "c"), onward(reach)))
        held += [(step, 0, same[-1]), (-step, 1, swap(same[-1]))]
        held += [(step, 1, cross[-1]), (-step, 0, swap(cross[-1]))]
    far = lax.ppermute(same[2], ("z", "c"), onward(2))
    held += [(4, 0, far), (4, 1, swap(far))]
    held[13], held[14] = held[14], held[13]

    queries = [q] + [lax.ppermute(q, "y", shift(Y, s)) for s in (1, 2, 3)]

    toward = 2 * c - 1
    column = jnp.stack(
        [((z + toward * d) % Z) * (Y * C) + y * C + (c ^ cc) for d, cc, _ in held]
    ).astype(jnp.int32)
    picks = [a[rows:].astype(jnp.float32).astype(jnp.int32) for a in queries]
    owner = jnp.stack([a[0, :count] for a in picks])[:, None, :]
    local = jnp.stack([a[1, :count] for a in picks])[:, None, :]
    row = jnp.arange(count, dtype=jnp.int32) // chosen_owner.shape[1]
    hit = owner == column[None, :, None]
    table = jnp.sum(jnp.where(hit, 1 + 8 * row + local, 0), axis=2)

    arrays = [a for _, _, a in held]
    carry, begin = (), 0
    for name, end in (("early", 10), ("middle", 12), ("nearly", 14), ("late", Z * C)):
        parts = attend(table, begin, queries, arrays[begin:end], carry, name == "late", blocks)
        carry, begin = parts[-1:], end

    back = [parts[0]] + [lax.ppermute(parts[s], "y", shift(Y, -s)) for s in (1, 2, 3)]
    attended = merge(back, blocks)
    spread = [attended] + [lax.ppermute(attended, "x", shift(X, s)) for s in (1, 2, 3)]
    started = open_output(attended, weights[0])
    return finish(started, spread[1:], weights[1:])


def solution(mesh):
    fine = Mesh(mesh.devices.reshape(Z, Y, C, X), ("z", "y", "c", "x"))
    kv = ("z", "y", "c")
    return jax.shard_map(
        on_device,
        mesh=fine,
        in_specs=(
            P(kv, "x"),
            P(None, "x"),
            P(None, "x"),
            P(None, "x"),
            P("x", None),
            P("x"),
            P(kv, None),
            P(kv, None),
        ),
        out_specs=P(kv, "x"),
        check_vma=False,
    )
```
